32 devices in a mesh: rep: 2 (over x), fs: 8 (over z, y), tp: 2 (over core).
Axes of the slice: x: 2, y: 2, z: 4, core: 2. Of those that a mesh axis runs over, the one named last changes fastest.
Arguments:
- tokens: bfloat16 [6144, 2048], P(('rep', 'fs'), 'tp'), may hold values from -6 to 6
- mix_gain: float32 [2048], replicated, may hold values from 0.1 to 1.9
- w_u: bfloat16 [2048, 2048], P('fs', 'tp'), may hold values from -0.125 to 0.125
- w_v: bfloat16 [2048, 2048], P('fs', 'tp'), may hold values from -0.125 to 0.125
- norm_gain: float32 [2048], P('tp'), may hold values from 0.1 to 1.9
- mix_weight: bfloat16 [16, 128, 128], P('tp'), may hold values from -0.5 to 0.5
- mix_bias: float32 [16, 128], P('tp'), may hold values from 0.1 to 1.9
- w_mix_out: bfloat16 [2048, 2048], P('tp', 'fs'), may hold values from -0.125 to 0.125
- ffn_gain: float32 [2048], replicated, may hold values from 0.1 to 1.9
- w_gate: bfloat16 [2048, 3072], P('fs', 'tp'), may hold values from -0.125 to 0.125
- w_value: bfloat16 [2048, 3072], P('fs', 'tp'), may hold values from -0.125 to 0.125
- taps_gate: bfloat16 [3, 3072], P(None, 'tp'), may hold values from -3.5 to 3.5
- taps_value: bfloat16 [3, 3072], P(None, 'tp'), may hold values from -3.5 to 3.5
- w_down: bfloat16 [3072, 2048], P('tp', 'fs'), may hold values from -0.109375 to 0.109375
Outputs:
- layer_out: bfloat16 [6144, 2048], P(('rep', 'fs'), 'tp')
The draws below stay inside these ranges and needn't reach their ends.
All inputs are finite; a program needn't handle non-finite values.
Results may differ from the reference program's by a relative error of at most 0.017.
Values may be sent and summed in bfloat16 or wider, within the bound.
A program may use at most 64 MiB of HBM per device.

```python
import jax
import jax.numpy as jnp
from jax import lax

D = 2048
GROUPS = 16
MIX_WIDTH = 2048
FF = 3072
BLOCK = 128
CONV = 3
TOK_DEV = 384
TOKENS = 6144
N_TP = 2


def level_of(rng, extent, split, low, top_value):
    level, own = 1.0, jax.random.fold_in(rng, 6)
    for dim, blocks in split:
        draws = jnp.exp(jax.random.uniform(jax.random.fold_in(own, dim), (blocks,), jnp.float32, low / len(split), top_value / len(split)))
        level = level * jnp.repeat(draws, extent[dim] // blocks).reshape([-1 if axis == dim else 1 for axis in range(len(extent))])
    return level


def scatter_about(own_key, extent, deviation, most, pieces=(), kind=jnp.bfloat16):
    drawn = jax.random.normal(own_key, extent, jnp.float32) * deviation
    if len(pieces) > 0:
        drawn = level_of(own_key, extent, pieces, -0.22, 0.18) * drawn
    return jnp.clip(drawn, min=-most, max=most).astype(kind)


def setup_inputs(seed: int = 0) -> dict:
    key_of = jax.random.split(jax.random.key(seed), 15)
    tokens = scatter_about(key_of[0], (TOKENS, D), 1.0, 6.0, ((0, 16), (1, 2)))
    mix_gain = jnp.clip(1.0 + 0.18 * jax.random.normal(key_of[1], (D,), jnp.float32), 0.1, 1.9)
    w_u = scatter_about(key_of[2], (D, MIX_WIDTH), D ** -0.5, 0.125, ((0, 8), (1, 2)))
    w_v = scatter_about(key_of[3], (D, MIX_WIDTH), D ** -0.5, 0.125, ((0, 8), (1, 2)))
    norm_gain = jnp.clip(1.0 + 0.18 * jax.random.normal(key_of[4], (MIX_WIDTH,), jnp.float32), 0.1, 1.9)
    mix_weight = scatter_about(key_of[5], (GROUPS, BLOCK, BLOCK), BLOCK ** -0.5, 0.5, ((0, 2),))
    mix_bias = jnp.clip(1.0 + 0.18 * jax.random.normal(key_of[6], (GROUPS, BLOCK), jnp.float32), 0.1, 1.9)
    w_mix_out = scatter_about(key_of[7], (MIX_WIDTH, D), MIX_WIDTH ** -0.5, 0.125, ((0, 2), (1, 8)))
    ffn_gain = jnp.clip(1.0 + 0.18 * jax.random.normal(key_of[8], (D,), jnp.float32), 0.1, 1.9)
    w_gate = scatter_about(key_of[9], (D, FF), D ** -0.5, 0.125, ((0, 8), (1, 2)))
    w_value = scatter_about(key_of[10], (D, FF), D ** -0.5, 0.125, ((0, 8), (1, 2)))
    taps_gate = scatter_about(key_of[11], (CONV, FF), CONV ** -0.5, 3.5, ((1, 2),))
    taps_value = scatter_about(key_of[12], (CONV, FF), CONV ** -0.5, 3.5, ((1, 2),))
    w_down = scatter_about(key_of[13], (FF, D), FF ** -0.5, 0.109375, ((0, 2), (1, 8)))
    return {"tokens": tokens, "mix_gain": mix_gain, "w_u": w_u, "w_v": w_v, "norm_gain": norm_gain, "mix_weight": mix_weight, "mix_bias": mix_bias, "w_mix_out": w_mix_out, "ffn_gain": ffn_gain, "w_gate": w_gate, "w_value": w_value, "taps_gate": taps_gate, "taps_value": taps_value, "w_down": w_down}


EPS_RMS = 1e-06
EPS_LN = 1e-05

def rms_scale(features, gain_vec):
    values = features.astype(jnp.float32)
    scaled = values * lax.rsqrt(lax.optimization_barrier(jnp.mean(values * values, axis=-1, keepdims=True)) + EPS_RMS)
    return (scaled * gain_vec).astype(jnp.bfloat16)

def spatial_mix(u_pre, v_pre, norm_gain, mix_weight, mix_bias):
    row_count = u_pre.shape[0]
    groups = mix_weight.shape[0]
    block_len = mix_weight.shape[1]
    group_width = v_pre.shape[1] // groups
    activated = jax.nn.gelu(v_pre).reshape(row_count, groups, group_width)
    average = lax.optimization_barrier(jnp.mean(activated, axis=-1, keepdims=True))
    spread_sq = lax.optimization_barrier(jnp.mean(jnp.square(activated - average), axis=-1, keepdims=True))
    v_norm = ((activated - average) * lax.rsqrt(spread_sq + EPS_LN) * norm_gain.reshape(groups, group_width)).astype(jnp.bfloat16)
    blocks = v_norm.reshape(row_count // block_len, block_len, groups, group_width)
    lower_mask = jnp.arange(block_len)[:, None] >= jnp.arange(block_len)[None, :]
    masked = jnp.where(lower_mask[None], mix_weight, jnp.zeros_like(mix_weight))
    mixed_rows = jnp.einsum('gts,nsgc->ntgc', masked.astype(jnp.float32), blocks.astype(jnp.float32))
    mixed_rows = mixed_rows + jnp.transpose(mix_bias)[None, :, :, None]
    mixed_rows = mixed_rows.reshape(row_count, groups * group_width)
    return (jax.nn.gelu(u_pre) * mixed_rows).astype(jnp.bfloat16)

def causal_taps(values, tap_weights, seq_len):
    row_count, channels = values.shape
    conv_len = tap_weights.shape[0]
    sequences = values.reshape(row_count // seq_len, seq_len, channels)
    padded = jnp.pad(sequences, ((0, 0), (conv_len - 1, 0), (0, 0)))
    summed_terms = jnp.zeros_like(sequences)
    for tap_index in range(conv_len):
        summed_terms = summed_terms + tap_weights[tap_index].astype(jnp.float32) * padded[:, tap_index:tap_index + seq_len]
    return summed_terms.reshape(row_count, channels)

def split_sum(operand, weight):
    share_width = operand.shape[1] // N_TP
    summed_terms = jnp.zeros((operand.shape[0], weight.shape[1]), jnp.float32)
    for member in range(N_TP):
        partial_value = jnp.dot(operand[:, member * share_width:(member + 1) * share_width], weight[member * share_width:(member + 1) * share_width], preferred_element_type=jnp.float32)
        rounded = lax.optimization_barrier(partial_value.astype(jnp.bfloat16))
        summed_terms = summed_terms + rounded.astype(jnp.float32)
    return summed_terms

def reference(tokens, mix_gain, w_u, w_v, norm_gain, mix_weight, mix_bias, w_mix_out, ffn_gain, w_gate, w_value, taps_gate, taps_value, w_down):
    normed = rms_scale(tokens, mix_gain)
    u_pre = jnp.dot(normed, w_u, preferred_element_type=jnp.float32)
    v_pre = jnp.dot(normed, w_v, preferred_element_type=jnp.float32)
    hidden = spatial_mix(u_pre, v_pre, norm_gain, mix_weight, mix_bias)
    middle = (tokens.astype(jnp.float32) + split_sum(hidden, w_mix_out)).astype(jnp.bfloat16)
    normed_mid = rms_scale(middle, ffn_gain)
    gate_pre = jnp.dot(normed_mid, w_gate, preferred_element_type=jnp.float32)
    value_pre = jnp.dot(normed_mid, w_value, preferred_element_type=jnp.float32)
    gate_conv = causal_taps(gate_pre, taps_gate, TOK_DEV)
    value_conv = causal_taps(value_pre, taps_value, TOK_DEV)
    activation = (jax.nn.gelu(gate_conv) * value_conv).astype(jnp.bfloat16)
    return (middle.astype(jnp.float32) + split_sum(activation, w_down)).astype(jnp.bfloat16)
```

```python
import jax
import jax.numpy as jnp
from jax import lax
from jax.sharding import PartitionSpec as P

EPS_RMS = 1e-06
EPS_LN = 1e-05


def rms_scale(features, gain_vec):
    values = features.astype(jnp.float32)
    scaled = values * lax.rsqrt(jnp.mean(values * values, axis=-1, keepdims=True) + EPS_RMS)
    return (scaled * gain_vec).astype(jnp.bfloat16)


def spatial_mix(u_pre, v_pre, norm_gain, mix_weight, mix_bias):
    row_count = u_pre.shape[0]
    groups = mix_weight.shape[0]
    block_len = mix_weight.shape[1]
    group_width = v_pre.shape[1] // groups
    activated = jax.nn.gelu(v_pre).reshape(row_count, groups, group_width)
    average = jnp.mean(activated, axis=-1, keepdims=True)
    spread_sq = jnp.mean(jnp.square(activated - average), axis=-1, keepdims=True)
    v_norm = (
        (activated - average)
        * lax.rsqrt(spread_sq + EPS_LN)
        * norm_gain.reshape(groups, group_width)
    ).astype(jnp.bfloat16)
    blocks = v_norm.reshape(row_count // block_len, block_len, groups, group_width)
    lower_mask = jnp.arange(block_len)[:, None] >= jnp.arange(block_len)[None, :]
    masked = jnp.where(lower_mask[None], mix_weight, jnp.zeros_like(mix_weight))
    mixed_rows = jnp.einsum("gts,nsgc->ntgc", masked, blocks, preferred_element_type=jnp.float32)
    mixed_rows = mixed_rows + jnp.transpose(mix_bias)[None, :, :, None]
    mixed_rows = mixed_rows.reshape(row_count, groups * group_width)
    return (jax.nn.gelu(u_pre) * mixed_rows).astype(jnp.bfloat16)


def causal_taps(values, tap_weights):
    seq_len = values.shape[0]
    conv_len = tap_weights.shape[0]
    padded = jnp.pad(values, ((conv_len - 1, 0), (0, 0)))
    summed_terms = jnp.zeros_like(values)
    for tap_index in range(conv_len):
        summed_terms = (
            summed_terms
            + tap_weights[tap_index].astype(jnp.float32) * padded[tap_index : tap_index + seq_len]
        )
    return summed_terms


def add_pair(operand, pieces):
    first = jnp.dot(operand, pieces[0], preferred_element_type=jnp.float32)
    second = jnp.dot(operand, pieces[1], preferred_element_type=jnp.float32)
    return (first, second)


def project_with(operand, weight_piece):
    return jnp.dot(operand, weight_piece, preferred_element_type=jnp.float32)


def own_half(array, axis):
    share = array.shape[axis] // lax.axis_size("rep")
    return lax.dynamic_slice_in_dim(array, lax.axis_index("rep") * share, share, axis)


def share_tokens(own):
    return lax.all_gather(lax.all_gather(own, "rep", axis=0, tiled=True), "tp", axis=1, tiled=True)


def scatter_sums(terms):
    part = lax.psum_scatter(terms.astype(jnp.bfloat16), "tp", scatter_dimension=1, tiled=True)
    return lax.psum_scatter(part, "rep", scatter_dimension=0, tiled=True).astype(jnp.float32)


def on_device(
    tokens,
    mix_gain,
    w_u,
    w_v,
    norm_gain,
    mix_weight,
    mix_bias,
    w_mix_out,
    ffn_gain,
    w_gate,
    w_value,
    taps_gate,
    taps_value,
    w_down,
):
    seq_len = tokens.shape[0]
    features = share_tokens(tokens)
    w_in = lax.all_gather(
        jnp.concatenate((own_half(w_u, 1), own_half(w_v, 1)), 1), "fs", axis=0, tiled=True
    )
    w_out = lax.all_gather(own_half(w_mix_out, 0), "fs", axis=1, tiled=True)
    w_up = lax.all_gather(
        jnp.concatenate((own_half(w_gate, 1), own_half(w_value, 1)), 1), "fs", axis=0, tiled=True
    )
    w_dn = lax.all_gather(own_half(w_down, 0), "fs", axis=1, tiled=True)
    normed = rms_scale(features, mix_gain)
    u_pre, v_pre = jnp.split(project_with(normed, w_in), 2, 1)
    hidden = spatial_mix(
        u_pre, v_pre, own_half(norm_gain, 0), own_half(mix_weight, 0), own_half(mix_bias, 0)
    )
    mixer_own = scatter_sums(project_with(hidden, w_out))
    middle_own = (tokens.astype(jnp.float32) + mixer_own).astype(jnp.bfloat16)
    normed_mid = rms_scale(share_tokens(middle_own), ffn_gain)
    gate_pre, value_pre = jnp.split(project_with(normed_mid, w_up), 2, 1)
    sequences = (-1, seq_len, gate_pre.shape[1])
    conv = jax.vmap(causal_taps, (0, None))
    activation = (
        jax.nn.gelu(conv(gate_pre.reshape(sequences), own_half(taps_gate, 1)))
        * conv(value_pre.reshape(sequences), own_half(taps_value, 1))
    ).astype(jnp.bfloat16)
    activation = activation.reshape(gate_pre.shape)
    channel_own = scatter_sums(project_with(activation, w_dn))
    return (middle_own.astype(jnp.float32) + channel_own).astype(jnp.bfloat16)


def solution(mesh):
    placed = (
        P(("rep", "fs"), "tp"),
        P(),
        P("fs", "tp"),
        P("fs", "tp"),
        P("tp"),
        P("tp", None, None),
        P("tp", None),
        P("tp", "fs"),
        P(),
        P("fs", "tp"),
        P("fs", "tp"),
        P(None, "tp"),
        P(None, "tp"),
        P("tp", "fs"),
    )
    return jax.shard_map(
        on_device, mesh=mesh, in_specs=placed, out_specs=P(("rep", "fs"), "tp"), check_vma=False
    )
```

```python
import functools

import jax
import jax.numpy as jnp
from jax import lax
from jax.experimental import pallas as pl
from jax.experimental.pallas import tpu as pltpu
from jax.sharding import PartitionSpec as P

EPS_RMS = 1e-06
EPS_LN = 1e-05
F32 = jnp.float32
BF16 = jnp.bfloat16
MESH = pl.DeviceIdType.MESH


def own_half(array, axis):
    share = array.shape[axis] // lax.axis_size("rep")
    return lax.dynamic_slice_in_dim(array, lax.axis_index("rep") * share, share, axis)


def layer_kernel(
    n, nr, nt,
    tok, mix_gain, w_in, norm_gain, mixw, bias, w_out, ffn_gain, w_up, taps_g, taps_v, w_dn,
    out,
    g_in, g_out, g_up, g_dn, feat, feat2, normed, uv, hidden, gv, act, part1, part2, got1, got2,
    w_send, w_recv, w_local, f_send, f_recv, p_send, p_recv,
):
    rep, fs, tp = lax.axis_index("rep"), lax.axis_index("fs"), lax.axis_index("tp")
    seq, own_width = tok.shape
    nz = n // 2
    z, y = fs // 2, fs % 2
    per = n // nt
    depth = normed.shape[2]
    mine = (w_in, w_out, w_up, w_dn)
    gathered = (g_in, g_out, g_up, g_dn)
    offsets = [(a, b) for a in range(nr) for b in range(nt) if (a, b) != (0, 0)]

    def peer(a, b):
        return {"rep": lax.rem(rep + a, nr), "tp": lax.rem(tp + b, nt)}

    barrier = pltpu.get_barrier_semaphore()
    line = (lax.rem(z + 1, nz), lax.rem(z + nz - 1, nz))
    greeted = [{"fs": z * 2 + 1 - y}] + [{"fs": at * 2 + y} for at in line]
    greeted += [peer(a, b) for a, b in offsets]
    for target in greeted:
        pl.semaphore_signal(barrier, inc=1, device_id=target, device_id_type=MESH)
    pl.semaphore_wait(barrier, len(greeted))

    def hop(stage, block, way):
        target = (fs + 2, fs - 2, z * 2 + 1 - y)[way]
        return pltpu.make_async_remote_copy(
            src_ref=gathered[stage].at[block],
            dst_ref=gathered[stage].at[block],
            send_sem=w_send.at[stage, way, block],
            recv_sem=w_recv.at[stage, block],
            device_id={"fs": target},
            device_id_type=MESH,
        )

    def ways(src):
        return (
            jnp.logical_and(src <= z, z < nz - 1),
            jnp.logical_and(src >= z, z > 0),
        )

    def forward(stage, src):
        block = src * 2 + y
        hop(stage, block, 2).start()
        for way, used in enumerate(ways(src)):
            @pl.when(used)
            def _():
                hop(stage, block, way).start()

    def arrived(stage, block):
        hop(stage, block, 2).wait_recv()

    def order(i):
        near = jnp.minimum(z, nz - 1 - z)
        swing = z + ((i + 1) // 2) * (1 - 2 * (i % 2))
        rest = jnp.where(z < nz - 1 - z, i, nz - 1 - i)
        return jnp.where(i <= 2 * near, swing, rest)

    def stage_loop(stage, compute, begin, middle):
        def step(i, _):
            src = order(i)

            @pl.when(i > 0)
            def _():
                arrived(stage, src * 2 + y)
                forward(stage, src)

            compute(src * 2 + y)

            @pl.when(i > 0)
            def _():
                other = order(i - 1) * 2 + 1 - y
                arrived(stage, other)
                compute(other)

            return 0

        lax.fori_loop(begin, nz, step, 0)
        middle()
        last = order(nz - 1) * 2 + 1 - y
        arrived(stage, last)
        compute(last)

    locals_ = [
        pltpu.make_async_copy(mine[k], gathered[k].at[fs], w_local.at[k]) for k in range(4)
    ]
    own_tok = pltpu.make_async_copy(tok, feat.at[rep, tp], w_local.at[4])
    for copy in locals_ + [own_tok]:
        copy.start()

    def share(turn, slabs):
        copies = []
        for k, (a, b) in enumerate(offsets):
            copies.append(
                pltpu.make_async_remote_copy(
                    src_ref=slabs.at[rep, tp],
                    dst_ref=slabs.at[rep, tp],
                    send_sem=f_send.at[turn, k],
                    recv_sem=f_recv.at[turn, k],
                    device_id=peer(a, b),
                    device_id_type=MESH,
                )
            )
        return copies

    def share_wait(turn, slabs):
        for k, (a, b) in enumerate(offsets):
            slab = slabs.at[lax.rem(rep + nr - a, nr), lax.rem(tp + nt - b, nt)]
            pltpu.make_async_remote_copy(
                src_ref=slab, dst_ref=slab, send_sem=f_send.at[turn, k],
                recv_sem=f_recv.at[turn, k], device_id=peer(a, b), device_id_type=MESH,
            ).wait_recv()

    def norm(slabs, gain):
        for r in range(nr):
            total = jnp.zeros((seq, 1), F32)
            for t in range(nt):
                values = slabs[r, t].astype(F32)
                total += jnp.sum(values * values, axis=1, keepdims=True)
            scale = lax.rsqrt(total / (nt * own_width) + EPS_RMS)
            for t in range(nt):
                for j in range(per):
                    values = slabs[r, t, :, j * depth : (j + 1) * depth].astype(F32)
                    normed[t * per + j, r * seq : (r + 1) * seq, :] = (
                        values * scale * gain[t * per + j]
                    ).astype(BF16)

    def piece(turn, part, got, block, r):
        return pltpu.make_async_remote_copy(
            src_ref=part.at[block, r],
            dst_ref=got.at[rep * nt + tp, block % per],
            send_sem=p_send.at[turn, block, r],
            recv_sem=p_recv.at[turn, rep * nt + tp, block % per],
            device_id={"rep": r, "tp": block // per},
            device_id_type=MESH,
        )

    def abroad(block, r):
        return jnp.logical_or(block // per != tp, r != rep)

    def project(turn, left, gathered_w, part, got, block):
        for r in range(nr):
            part[block, r] = jnp.dot(
                left[r], gathered_w[block], preferred_element_type=F32
            ).astype(BF16)

            @pl.when(abroad(block, r))
            def _():
                piece(turn, part, got, block, r).start()

    def collect(turn, part, got, base, emit):
        for j in range(per):
            total = part[tp * per + j, rep].astype(F32)
            for a, b in offsets:
                slot = lax.rem(rep + a, nr) * nt + lax.rem(tp + b, nt)
                landing = got.at[slot, j]
                pltpu.make_async_remote_copy(
                    src_ref=landing, dst_ref=landing, send_sem=p_send.at[turn, 0, 0],
                    recv_sem=p_recv.at[turn, slot, j], device_id=peer(a, b),
                    device_id_type=MESH,
                ).wait_recv()
                total += got[slot, j].astype(F32)
            width = total.shape[1]
            span = slice(j * width, (j + 1) * width)
            emit(span, (base(span).astype(F32) + total).astype(BF16))

    for copy in locals_ + [own_tok]:
        copy.wait()
    for copy in share(0, feat):
        copy.start()
    forward(0, z)
    forward(1, z)
    uv[...] = jnp.zeros_like(uv)
    gv[...] = jnp.zeros_like(gv)
    share_wait(0, feat)
    norm(feat, mix_gain)

    def in_block(block):
        for r in range(nr):
            rows = slice(r * seq, (r + 1) * seq)
            uv[rows, :] += jnp.dot(
                normed[block, rows, :], g_in[block], preferred_element_type=F32
            )

    stage_loop(0, in_block, 0, lambda: forward(2, z))

    groups, block_len = mixw.shape[0], mixw.shape[1]
    group_width = uv.shape[1] // 2 // groups

    for r in range(nr):
        def mix_rows(i, _):
            start = pl.multiple_of(i * block_len, block_len)
            rows = pl.ds(pl.multiple_of(r * seq + i * block_len, block_len), block_len)
            for g in range(groups):
                at = g * group_width
                half = groups * group_width
                activated = jax.nn.gelu(uv[rows, half + at : half + at + group_width])
                centred = activated - jnp.mean(activated, axis=1, keepdims=True)
                spread = jnp.mean(centred * centred, axis=1, keepdims=True)
                v_norm = (
                    centred * lax.rsqrt(spread + EPS_LN) * norm_gain[:, at : at + group_width]
                ).astype(BF16)
                mixed = jnp.dot(mixw[g], v_norm, preferred_element_type=F32) + bias[g]
                hidden[r, pl.ds(start, block_len), at : at + group_width] = (
                    jax.nn.gelu(uv[rows, at : at + group_width]) * mixed
                ).astype(BF16)
            return 0

        lax.fori_loop(0, seq // block_len, mix_rows, 0)

    stage_loop(
        1, functools.partial(project, 0, hidden, g_out, part1, got1), 0, lambda: forward(3, z)
    )

    def relay(stage, begin, end):
        def step(i, _):
            arrived(stage, order(i) * 2 + y)
            forward(stage, order(i))
            return 0

        lax.fori_loop(begin, end, step, 0)

    def put_middle(span, value):
        feat2[rep, tp, :, span] = value

    relay(2, 1, nz // 2)
    collect(0, part1, got1, lambda span: tok[:, span], put_middle)
    for copy in share(1, feat2):
        copy.start()
    relay(2, nz // 2, nz)
    share_wait(1, feat2)
    norm(feat2, ffn_gain)

    def up_block(block):
        for r in range(nr):
            gv[r, 8:, :] += jnp.dot(
                normed[block, r * seq : (r + 1) * seq, :],
                g_up[block],
                preferred_element_type=F32,
            )

    def up_step(i, _):
        up_block(order(i) * 2 + y)

        @pl.when(i > 0)
        def _():
            arrived(3, order(i) * 2 + y)
            forward(3, order(i))

        other = order(i) * 2 + 1 - y
        arrived(2, other)
        up_block(other)
        return 0

    lax.fori_loop(0, nz, up_step, 0)

    units = act.shape[2]
    taps_len = taps_g.shape[0]
    chunk = 128 if units % 128 == 0 else units
    for r in range(nr):
        for at in range(0, units, chunk):
            gate = jnp.zeros((seq, chunk), F32)
            value = jnp.zeros((seq, chunk), F32)
            for k in range(taps_len):
                first = 8 - (taps_len - 1) + k
                gate += taps_g[k : k + 1, at : at + chunk] * gv[r, first : first + seq, at : at + chunk]
                value += (
                    taps_v[k : k + 1, at : at + chunk]
                    * gv[r, first : first + seq, units + at : units + at + chunk]
                )
            act[r, :, at : at + chunk] = (jax.nn.gelu(gate) * value).astype(BF16)

    down = functools.partial(project, 1, act, g_dn, part2, got2)

    def down_own(i, _):
        down(order(i) * 2 + y)
        return 0

    def down_other(i, _):
        arrived(3, order(i) * 2 + 1 - y)
        down(order(i) * 2 + 1 - y)
        return 0

    lax.fori_loop(0, nz, down_own, 0)
    lax.fori_loop(0, nz, down_other, 0)

    def put_out(span, value):
        out[:, span] = value

    collect(1, part2, got2, lambda span: feat2[rep, tp, :, span], put_out)

    for turn, slabs in enumerate((feat, feat2)):
        for copy in share(turn, slabs):
            copy.wait_send()

    def drain_pieces(block, _):
        for r in range(nr):
            @pl.when(abroad(block, r))
            def _():
                piece(0, part1, got1, block, r).wait_send()
                piece(1, part2, got2, block, r).wait_send()
        return 0

    lax.fori_loop(0, n, drain_pieces, 0)

    def drain_hops(src, _):
        for stage in range(4):
            hop(stage, src * 2 + y, 2).wait_send()
            for way, used in enumerate(ways(src)):
                @pl.when(used)
                def _():
                    hop(stage, src * 2 + y, way).wait_send()
        return 0

    lax.fori_loop(0, nz, drain_hops, 0)


def on_device(
    tokens,
    mix_gain,
    w_u,
    w_v,
    norm_gain,
    mix_weight,
    mix_bias,
    w_mix_out,
    ffn_gain,
    w_gate,
    w_value,
    taps_gate,
    taps_value,
    w_down,
):
    n, nr, nt = lax.axis_size("fs"), lax.axis_size("rep"), lax.axis_size("tp")
    seq, own_width = tokens.shape
    depth, per = own_width * nt // n, n // nt
    block_len = mix_weight.shape[1]
    lower_mask = jnp.arange(block_len)[:, None] >= jnp.arange(block_len)[None, :]
    mixw = own_half(mix_weight, 0)
    mixw = jnp.where(lower_mask[None], mixw, jnp.zeros_like(mixw))
    w_in = jnp.concatenate((own_half(w_u, 1), own_half(w_v, 1)), 1)
    w_up = jnp.concatenate((own_half(w_gate, 1), own_half(w_value, 1)), 1)
    w_out, w_dn = own_half(w_mix_out, 0), own_half(w_down, 0)
    operands = (
        tokens,
        mix_gain.reshape(n, 1, depth),
        w_in,
        own_half(norm_gain, 0)[None, :],
        mixw,
        own_half(mix_bias, 0)[:, :, None],
        w_out,
        ffn_gain.reshape(n, 1, depth),
        w_up,
        own_half(taps_gate, 1).astype(F32),
        own_half(taps_value, 1).astype(F32),
        w_dn,
    )
    vmem, sem = pltpu.VMEM, pltpu.SemaphoreType.DMA
    others = nr * nt - 1
    return pl.pallas_call(
        functools.partial(layer_kernel, n, nr, nt),
        out_shape=jax.ShapeDtypeStruct((seq, own_width), BF16),
        in_specs=[pl.BlockSpec(memory_space=vmem)] * len(operands),
        out_specs=pl.BlockSpec(memory_space=vmem),
        scratch_shapes=[
            vmem((n,) + w_in.shape, BF16),
            vmem((n,) + w_out.shape, BF16),
            vmem((n,) + w_up.shape, BF16),
            vmem((n,) + w_dn.shape, BF16),
            vmem((nr, nt, seq, own_width), BF16),
            vmem((nr, nt, seq, own_width), BF16),
            vmem((n, nr * seq, depth), BF16),
            vmem((nr * seq, w_in.shape[1]), F32),
            vmem((nr, seq, w_out.shape[0]), BF16),
            vmem((nr, seq + 8, w_up.shape[1]), F32),
            vmem((nr, seq, w_dn.shape[0]), BF16),
            vmem((n, nr, seq, depth), BF16),
            vmem((n, nr, seq, depth), BF16),
            vmem((nr * nt, per, seq, depth), BF16),
            vmem((nr * nt, per, seq, depth), BF16),
            sem((4, 3, n)),
            sem((4, n)),
            sem((5,)),
            sem((2, others)),
            sem((2, others)),
            sem((2, n, nr)),
            sem((2, nr * nt, per)),
        ],
        compiler_params=pltpu.CompilerParams(
            collective_id=0, has_side_effects=True, vmem_limit_bytes=67043328
        ),
    )(*operands)


def solution(mesh):
    placed = (
        P(("rep", "fs"), "tp"),
        P(),
        P("fs", "tp"),
        P("fs", "tp"),
        P("tp"),
        P("tp", None, None),
        P("tp", None),
        P("tp", "fs"),
        P(),
        P("fs", "tp"),
        P("fs", "tp"),
        P(None, "tp"),
        P(None, "tp"),
        P("tp", "fs"),
    )
    return jax.shard_map(
        on_device, mesh=mesh, in_specs=placed, out_specs=P(("rep", "fs"), "tp"), check_vma=False
    )
```

```python
import functools

import jax
import jax.numpy as jnp
from jax import lax
from jax.experimental import pallas as pl
from jax.experimental.pallas import tpu as pltpu
from jax.sharding import PartitionSpec as P

EPS_RMS = 1e-06
EPS_LN = 1e-05
F32 = jnp.float32
BF16 = jnp.bfloat16
MESH = pl.DeviceIdType.MESH


def own_half(array, axis):
    share = array.shape[axis] // lax.axis_size("rep")
    return lax.dynamic_slice_in_dim(array, lax.axis_index("rep") * share, share, axis)


def layer_kernel(
    n, nr, nt,
    tok, mix_gain, w_in, norm_gain, mixw, bias, w_out, ffn_gain, w_up, taps_g, taps_v, w_dn,
    out,
    g_in, g_out, g_up, g_dn, feat, feat2, normed, uv, hidden, gv, act, part1, part2, got1, got2,
    w_send, w_recv, w_local, f_send, f_recv, p_send, p_recv,
):
    rep, fs, tp = lax.axis_index("rep"), lax.axis_index("fs"), lax.axis_index("tp")
    seq, own_width = tok.shape
    nz = n // 2
    z, y = fs // 2, fs % 2
    per = n // nt
    depth = normed.shape[2]
    mine = (w_in, w_out, w_up, w_dn)
    gathered = (g_in, g_out, g_up, g_dn)
    offsets = [(a, b) for a in range(nr) for b in range(nt) if (a, b) != (0, 0)]

    def peer(a, b):
        return {"rep": lax.rem(rep + a, nr), "tp": lax.rem(tp + b, nt)}

    barrier = pltpu.get_barrier_semaphore()
    line = (lax.rem(z + 1, nz), lax.rem(z + nz - 1, nz))
    greeted = [{"fs": z * 2 + 1 - y}] + [{"fs": at * 2 + y} for at in line]
    greeted += [peer(a, b) for a, b in offsets]
    for target in greeted:
        pl.semaphore_signal(barrier, inc=1, device_id=target, device_id_type=MESH)
    pl.semaphore_wait(barrier, len(greeted))

    def hop(stage, block, way):
        target = (fs + 2, fs - 2, z * 2 + 1 - y)[way]
        return pltpu.make_async_remote_copy(
            src_ref=gathered[stage].at[block],
            dst_ref=gathered[stage].at[block],
            send_sem=w_send.at[stage, way, block],
            recv_sem=w_recv.at[stage, block],
            device_id={"fs": target},
            device_id_type=MESH,
        )

    def ways(src):
        return (
            jnp.logical_and(src <= z, z < nz - 1),
            jnp.logical_and(src >= z, z > 0),
        )

    def forward(stage, src):
        block = src * 2 + y
        hop(stage, block, 2).start()
        for way, used in enumerate(ways(src)):
            @pl.when(used)
            def _():
                hop(stage, block, way).start()

    def arrived(stage, block):
        hop(stage, block, 2).wait_recv()

    def order(i):
        near = jnp.minimum(z, nz - 1 - z)
        swing = z + ((i + 1) // 2) * (1 - 2 * (i % 2))
        rest = jnp.where(z < nz - 1 - z, i, nz - 1 - i)
        return jnp.where(i <= 2 * near, swing, rest)

    def stage_loop(stage, compute, begin, middle):
        def step(i, _):
            src = order(i)

            @pl.when(i > 0)
            def _():
                arrived(stage, src * 2 + y)
                forward(stage, src)

            compute(src * 2 + y)

            @pl.when(i > 0)
            def _():
                other = order(i - 1) * 2 + 1 - y
                arrived(stage, other)
                compute(other)

            return 0

        lax.fori_loop(begin, nz, step, 0)
        middle()
        last = order(nz - 1) * 2 + 1 - y
        arrived(stage, last)
        compute(last)

    locals_ = [
        pltpu.make_async_copy(mine[k], gathered[k].at[fs], w_local.at[k]) for k in range(4)
    ]
    own_tok = pltpu.make_async_copy(tok, feat.at[rep, tp], w_local.at[4])
    for copy in locals_ + [own_tok]:
        copy.start()

    def share(turn, slabs):
        copies = []
        for k, (a, b) in enumerate(offsets):
            copies.append(
                pltpu.make_async_remote_copy(
                    src_ref=slabs.at[rep, tp],
                    dst_ref=slabs.at[rep, tp],
                    send_sem=f_send.at[turn, k],
                    recv_sem=f_recv.at[turn, k],
                    device_id=peer(a, b),
                    device_id_type=MESH,
                )
            )
        return copies

    def share_wait(turn, slabs):
        for k, (a, b) in enumerate(offsets):
            slab = slabs.at[lax.rem(rep + nr - a, nr), lax.rem(tp + nt - b, nt)]
            pltpu.make_async_remote_copy(
                src_ref=slab, dst_ref=slab, send_sem=f_send.at[turn, k],
                recv_sem=f_recv.at[turn, k], device_id=peer(a, b), device_id_type=MESH,
            ).wait_recv()

    def norm(slabs, gain):
        for r in range(nr):
            total = jnp.zeros((seq, 1), F32)
            for t in range(nt):
                values = slabs[r, t].astype(F32)
                total += jnp.sum(values * values, axis=1, keepdims=True)
            scale = lax.rsqrt(total / (nt * own_width) + EPS_RMS)
            for t in range(nt):
                for j in range(per):
                    values = slabs[r, t, :, j * depth : (j + 1) * depth].astype(F32)
                    normed[t * per + j, r * seq : (r + 1) * seq, :] = (
                        values * scale * gain[t * per + j]
                    ).astype(BF16)

    def piece(turn, part, got, block, r):
        return pltpu.make_async_remote_copy(
            src_ref=part.at[block, r],
            dst_ref=got.at[rep * nt + tp, block % per],
            send_sem=p_send.at[turn, block, r],
            recv_sem=p_recv.at[turn, rep * nt + tp, block % per],
            device_id={"rep": r, "tp": block // per},
            device_id_type=MESH,
        )

    def abroad(block, r):
        return jnp.logical_or(block // per != tp, r != rep)

    def project(turn, left, gathered_w, part, got, block):
        for r in range(nr):
            part[block, r] = jnp.dot(
                left[r], gathered_w[block], preferred_element_type=F32
            ).astype(BF16)

            @pl.when(abroad(block, r))
            def _():
                piece(turn, part, got, block, r).start()

    def collect(turn, part, got, base, emit):
        for j in range(per):
            total = part[tp * per + j, rep].astype(F32)
            for a, b in offsets:
                slot = lax.rem(rep + a, nr) * nt + lax.rem(tp + b, nt)
                landing = got.at[slot, j]
                pltpu.make_async_remote_copy(
                    src_ref=landing, dst_ref=landing, send_sem=p_send.at[turn, 0, 0],
                    recv_sem=p_recv.at[turn, slot, j], device_id=peer(a, b),
                    device_id_type=MESH,
                ).wait_recv()
                total += got[slot, j].astype(F32)
            width = total.shape[1]
            span = slice(j * width, (j + 1) * width)
            emit(span, (base(span).astype(F32) + total).astype(BF16))

    for copy in locals_ + [own_tok]:
        copy.wait()
    for copy in share(0, feat):
        copy.start()
    forward(0, z)
    forward(1, z)
    forward(2, z)
    uv[...] = jnp.zeros_like(uv)
    gv[...] = jnp.zeros_like(gv)
    share_wait(0, feat)
    norm(feat, mix_gain)

    def in_block(block):
        for r in range(nr):
            rows = slice(r * seq, (r + 1) * seq)
            uv[rows, :] += jnp.dot(
                normed[block, rows, :], g_in[block], preferred_element_type=F32
            )

    stage_loop(0, in_block, 0, lambda: forward(3, z))

    groups, block_len = mixw.shape[0], mixw.shape[1]
    group_width = uv.shape[1] // 2 // groups

    for r in range(nr):
        def mix_rows(i, _):
            start = pl.multiple_of(i * block_len, block_len)
            rows = pl.ds(pl.multiple_of(r * seq + i * block_len, block_len), block_len)
            for g in range(groups):
                at = g * group_width
                half = groups * group_width
                activated = jax.nn.gelu(uv[rows, half + at : half + at + group_width])
                centred = activated - jnp.mean(activated, axis=1, keepdims=True)
                spread = jnp.mean(centred * centred, axis=1, keepdims=True)
                v_norm = (
                    centred * lax.rsqrt(spread + EPS_LN) * norm_gain[:, at : at + group_width]
                ).astype(BF16)
                mixed = jnp.dot(mixw[g], v_norm, preferred_element_type=F32) + bias[g]
                hidden[r, pl.ds(start, block_len), at : at + group_width] = (
                    jax.nn.gelu(uv[rows, at : at + group_width]) * mixed
                ).astype(BF16)
            return 0

        lax.fori_loop(0, seq // block_len, mix_rows, 0)

    stage_loop(
        1, functools.partial(project, 0, hidden, g_out, part1, got1), 0, lambda: None
    )

    def relay(stage, begin, end):
        def step(i, _):
            arrived(stage, order(i) * 2 + y)
            forward(stage, order(i))
            return 0

        lax.fori_loop(begin, end, step, 0)

    def put_middle(span, value):
        feat2[rep, tp, :, span] = value

    relay(2, 1, nz // 2)
    collect(0, part1, got1, lambda span: tok[:, span], put_middle)
    for copy in share(1, feat2):
        copy.start()
    relay(2, nz // 2, nz)
    share_wait(1, feat2)
    norm(feat2, ffn_gain)

    def up_block(block):
        for r in range(nr):
            gv[r, 8:, :] += jnp.dot(
                normed[block, r * seq : (r + 1) * seq, :],
                g_up[block],
                preferred_element_type=F32,
            )

    def up_step(i, _):
        up_block(order(i) * 2 + y)

        @pl.when(i > 0)
        def _():
            arrived(3, order(i) * 2 + y)
            forward(3, order(i))

        other = order(i) * 2 + 1 - y
        arrived(2, other)
        up_block(other)
        return 0

    lax.fori_loop(0, nz, up_step, 0)

    units = act.shape[2]
    taps_len = taps_g.shape[0]
    chunk = 128 if units % 128 == 0 else units
    for r in range(nr):
        for at in range(0, units, chunk):
            gate = jnp.zeros((seq, chunk), F32)
            value = jnp.zeros((seq, chunk), F32)
            for k in range(taps_len):
                first = 8 - (taps_len - 1) + k
                gate += taps_g[k : k + 1, at : at + chunk] * gv[r, first : first + seq, at : at + chunk]
                value += (
                    taps_v[k : k + 1, at : at + chunk]
                    * gv[r, first : first + seq, units + at : units + at + chunk]
                )
            act[r, :, at : at + chunk] = (jax.nn.gelu(gate) * value).astype(BF16)

    down = functools.partial(project, 1, act, g_dn, part2, got2)

    def down_own(i, _):
        down(order(i) * 2 + y)
        return 0

    def down_other(i, _):
        arrived(3, order(i) * 2 + 1 - y)
        down(order(i) * 2 + 1 - y)
        return 0

    lax.fori_loop(0, nz, down_own, 0)
    lax.fori_loop(0, nz, down_other, 0)

    def put_out(span, value):
        out[:, span] = value

    collect(1, part2, got2, lambda span: feat2[rep, tp, :, span], put_out)

    for turn, slabs in enumerate((feat, feat2)):
        for copy in share(turn, slabs):
            copy.wait_send()

    def drain_pieces(block, _):
        for r in range(nr):
            @pl.when(abroad(block, r))
            def _():
                piece(0, part1, got1, block, r).wait_send()
                piece(1, part2, got2, block, r).wait_send()
        return 0

    lax.fori_loop(0, n, drain_pieces, 0)

    def drain_hops(src, _):
        for stage in range(4):
            hop(stage, src * 2 + y, 2).wait_send()
            for way, used in enumerate(ways(src)):
                @pl.when(used)
                def _():
                    hop(stage, src * 2 + y, way).wait_send()
        return 0

    lax.fori_loop(0, nz, drain_hops, 0)


def on_device(
    tokens,
    mix_gain,
    w_u,
    w_v,
    norm_gain,
    mix_weight,
    mix_bias,
    w_mix_out,
    ffn_gain,
    w_gate,
    w_value,
    taps_gate,
    taps_value,
    w_down,
):
    n, nr, nt = lax.axis_size("fs"), lax.axis_size("rep"), lax.axis_size("tp")
    seq, own_width = tokens.shape
    depth, per = own_width * nt // n, n // nt
    block_len = mix_weight.shape[1]
    lower_mask = jnp.arange(block_len)[:, None] >= jnp.arange(block_len)[None, :]
    mixw = own_half(mix_weight, 0)
    mixw = jnp.where(lower_mask[None], mixw, jnp.zeros_like(mixw))
    w_in = jnp.concatenate((own_half(w_u, 1), own_half(w_v, 1)), 1)
    w_up = jnp.concatenate((own_half(w_gate, 1), own_half(w_value, 1)), 1)
    w_out, w_dn = own_half(w_mix_out, 0), own_half(w_down, 0)
    operands = (
        tokens,
        mix_gain.reshape(n, 1, depth),
        w_in,
        own_half(norm_gain, 0)[None, :],
        mixw,
        own_half(mix_bias, 0)[:, :, None],
        w_out,
        ffn_gain.reshape(n, 1, depth),
        w_up,
        own_half(taps_gate, 1).astype(F32),
        own_half(taps_value, 1).astype(F32),
        w_dn,
    )
    vmem, sem = pltpu.VMEM, pltpu.SemaphoreType.DMA
    others = nr * nt - 1
    return pl.pallas_call(
        functools.partial(layer_kernel, n, nr, nt),
        out_shape=jax.ShapeDtypeStruct((seq, own_width), BF16),
        in_specs=[pl.BlockSpec(memory_space=vmem)] * len(operands),
        out_specs=pl.BlockSpec(memory_space=vmem),
        scratch_shapes=[
            vmem((n,) + w_in.shape, BF16),
            vmem((n,) + w_out.shape, BF16),
            vmem((n,) + w_up.shape, BF16),
            vmem((n,) + w_dn.shape, BF16),
            vmem((nr, nt, seq, own_width), BF16),
            vmem((nr, nt, seq, own_width), BF16),
            vmem((n, nr * seq, depth), BF16),
            vmem((nr * seq, w_in.shape[1]), F32),
            vmem((nr, seq, w_out.shape[0]), BF16),
            vmem((nr, seq + 8, w_up.shape[1]), F32),
            vmem((nr, seq, w_dn.shape[0]), BF16),
            vmem((n, nr, seq, depth), BF16),
            vmem((n, nr, seq, depth), BF16),
            vmem((nr * nt, per, seq, depth), BF16),
            vmem((nr * nt, per, seq, depth), BF16),
            sem((4, 3, n)),
            sem((4, n)),
            sem((5,)),
            sem((2, others)),
            sem((2, others)),
            sem((2, n, nr)),
            sem((2, nr * nt, per)),
        ],
        compiler_params=pltpu.CompilerParams(
            collective_id=0, has_side_effects=True, vmem_limit_bytes=67043328
        ),
    )(*operands)


def solution(mesh):
    placed = (
        P(("rep", "fs"), "tp"),
        P(),
        P("fs", "tp"),
        P("fs", "tp"),
        P("tp"),
        P("tp", None, None),
        P("tp", None),
        P("tp", "fs"),
        P(),
        P("fs", "tp"),
        P("fs", "tp"),
        P(None, "tp"),
        P(None, "tp"),
        P("tp", "fs"),
    )
    return jax.shard_map(
        on_device, mesh=mesh, in_specs=placed, out_specs=P(("rep", "fs"), "tp"), check_vma=False
    )
```
